128 devices in a mesh: ep: 64 (over z, y, x), tp: 2 (over core).
Axes of the slice: x: 4, y: 4, z: 4, core: 2. Of those that a mesh axis runs over, the one named last changes fastest.
Arguments:
- tokens: bfloat16 [12288, 2048], P('ep', 'tp'), may hold values from -6 to 6
- chosen: int32 [64, 1536], P('ep'), may hold values from 0 to 12287, as said below
- gate_score: float32 [64, 1536], P('ep'), may hold values from 0.1 to 1
- gate_weight: bfloat16 [64, 2048, 2048], P('ep', None, 'tp'), may hold values from -0.125 to 0.125
- up_weight: bfloat16 [64, 2048, 2048], P('ep', None, 'tp'), may hold values from -0.125 to 0.125
- down_weight: bfloat16 [64, 2048, 2048], P('ep', 'tp'), may hold values from -0.125 to 0.125
Outputs:
- mixed: bfloat16 [12288, 2048], P('ep', 'tp')
The draws below stay inside these ranges and needn't reach their ends.
Inputs may be any that keep to these rules, and one draw needn't show every extreme that they name: For every expert and every s, columns s * 24 to (s + 1) * 24 - 1 of chosen name 24 different tokens, all among tokens s * 192 to (s + 1) * 192 - 1.
All inputs are finite; a program needn't handle non-finite values.
Results may differ from the reference program's by a relative error of at most 0.012.
Values may be sent and summed in bfloat16 or wider, within the bound.
A program may use at most 128 MiB of HBM per device.

```python
import math
import jax
import jax.numpy as jnp
from jax import lax

D = 2048
FF = 2048
TOK_DEV = 192
PICK = 24
EXPERTS = 64
TOKENS = 12288
CAP = 1536
N_TP = 2


def draw_chosen(key, part):
    all_keys = jax.random.split(key, EXPERTS * EXPERTS)
    drawn = jax.vmap(lambda k: jax.random.permutation(k, TOK_DEV)[:PICK])(all_keys)
    drawn = drawn.reshape(EXPERTS, EXPERTS, PICK).astype(jnp.int32)
    block_start = (jnp.arange(EXPERTS, dtype=jnp.int32) * TOK_DEV)[None, :, None]
    return (drawn + block_start).reshape(EXPERTS, CAP).astype(jnp.int32)


def steps_of(own_key, shape, pieces, least, largest):
    gain = 1.0
    for dim, blocks in pieces:
        draws = jax.random.uniform(jax.random.fold_in(jax.random.fold_in(own_key, 6), dim), (blocks,), jnp.float32, least / len(pieces), largest / len(pieces))
        gain = gain * jnp.repeat(jnp.exp(draws), shape[dim] // blocks).reshape((-1,) + (1,) * (len(shape) - 1 - dim))
    return gain


def gaussian(rng, shape, width, bound, cuts=(), kind=jnp.bfloat16):
    values = jax.random.normal(rng, shape, jnp.float32) * width
    if len(cuts) > 0:
        values = steps_of(rng, shape, cuts, -0.22, 0.18) * values
    return jnp.clip(values, min=-bound, max=bound).astype(kind)


def setup_inputs(seed: int = 0) -> dict:
    key_of = jax.random.split(jax.random.key(seed), 7)
    tokens = gaussian(key_of[0], (TOKENS, D), 1.0, 6.0, ((0, 64), (1, 2)))
    chosen = draw_chosen(jax.random.fold_in(key_of[6], 71), 0)
    gate_score = jnp.clip(jnp.exp(math.log(1.0) - 2.3025851 * jax.random.uniform(key_of[2], (EXPERTS, CAP), jnp.float32) ** steps_of(key_of[2], (EXPERTS, CAP), ((0, 64),), -0.2, 0.2)), 0.1, 1.0)
    gate_weight = gaussian(key_of[3], (EXPERTS, D, FF), D ** -0.5, 0.125, ((0, 64), (2, 2)))
    up_weight = gaussian(key_of[4], (EXPERTS, D, FF), D ** -0.5, 0.125, ((0, 64), (2, 2)))
    down_weight = gaussian(key_of[5], (EXPERTS, FF, D), FF ** -0.5, 0.125, ((0, 64), (1, 2)))
    return dict(tokens=tokens, chosen=chosen, gate_score=gate_score, gate_weight=gate_weight, up_weight=up_weight, down_weight=down_weight)


def reference(tokens, chosen, gate_score, gate_weight, up_weight, down_weight):
    ff_part = FF // N_TP

    def expert_step(total, inputs):
        token_ids, scores, w_gate, w_up, w_down = inputs
        picked = jnp.take(tokens, token_ids, axis=0)
        gate_pre = jnp.dot(picked, w_gate, preferred_element_type=jnp.float32)
        up_pre = jnp.dot(picked, w_up, preferred_element_type=jnp.float32)
        hidden = (jax.nn.silu(gate_pre) * up_pre).astype(jnp.bfloat16)
        summed = jnp.zeros((CAP, D), jnp.float32)
        for shard_index in range(N_TP):
            lower = shard_index * ff_part
            partial_value = jnp.dot(hidden[:, lower:lower + ff_part], w_down[lower:lower + ff_part],
                              preferred_element_type=jnp.float32).astype(jnp.bfloat16)
            summed = summed + lax.optimization_barrier(partial_value).astype(jnp.float32)
        weighted = (summed * scores[:, None]).astype(jnp.bfloat16)
        total = total.at[token_ids].add(lax.optimization_barrier(weighted).astype(jnp.float32))
        return total, None

    start_total = jnp.zeros((TOKENS, D), jnp.float32)
    total, _ = lax.scan(expert_step, start_total, (chosen, gate_score, gate_weight, up_weight, down_weight))
    return total.astype(jnp.bfloat16)
```

```python
import jax
import jax.numpy as jnp
from jax import lax
from jax.experimental import pallas as pl
from jax.experimental.pallas import tpu as pltpu
from jax.sharding import PartitionSpec as P

BF16 = jnp.bfloat16
F32 = jnp.float32
MESH = pl.DeviceIdType.MESH
TOK = 192
PICK = 24
HALF = 1024
ROWS = 16 * PICK
SLICES = ((0, 384), (384, 384), (768, 256))


def offset_of(s, a, b, c):
    if s == 0:
        return c, a, b
    if s == 1:
        return a, c, b
    return a, b, c


def kernel(
    tokens, chosen, score, wg_hbm, wu_hbm, wd_hbm, out,
    wg, wu, wd, gathered, isend, irecv, pick, dsend, own, other, hidden, pown, psend, precv,
    wt, ret, sums, rsend, rrecv, scale,
    w_sem, i_send, i_recv, g_send, g_recv, d_send, d_recv, f_send, f_recv, p_send, p_recv,
    r_send, r_recv, q_send, q_recv,
):
    ep = lax.axis_index("ep")
    tp = lax.axis_index("tp")
    z, y, x = ep // 16, (ep // 4) % 4, ep % 4

    def peer(dz, dy, dx):
        return ((z + dz + 4) % 4) * 16 + ((y + dy + 4) % 4) * 4 + (x + dx + 4) % 4

    def remote(src, dst, send, recv, dev):
        return pltpu.make_async_remote_copy(
            src_ref=src, dst_ref=dst, send_sem=send, recv_sem=recv, device_id=dev, device_id_type=MESH
        )

    partner = (ep, 1 - tp)

    def block_of(s, a, b, c):
        dz, dy, dx = offset_of(s, a, b, c)
        return dy * 4 + dx

    weights = [
        pltpu.make_async_copy(src, dst, w_sem.at[i])
        for i, (src, dst) in enumerate(((wg_hbm, wg), (wu_hbm, wu), (wd_hbm, wd)))
    ]
    for copy in weights:
        copy.start()

    barrier = pltpu.get_barrier_semaphore()
    near = 0
    for dz in range(4):
        for dy in range(4):
            for dx in range(4):
                if (dz or dy or dx) and not (dz and dy and dx):
                    near += 1
                    pl.semaphore_signal(barrier, 1, device_id=(peer(dz, dy, dx), tp), device_id_type=MESH)
    pl.semaphore_signal(barrier, 1, device_id=partner, device_id_type=MESH)

    lane = lax.broadcasted_iota(jnp.int32, (64, 128), 1)
    local = chosen[...] - TOK * lax.broadcasted_iota(jnp.int32, (64, 128), 0) + 1
    local = jnp.where(lane < PICK, local, 0).astype(F32)
    shifted = jnp.concatenate(
        [local if a == 0 else pltpu.roll(local, a * PICK, 1) for a in range(4)], axis=0
    ).astype(BF16)
    row = lax.broadcasted_iota(jnp.int32, (128, 256), 0)
    col = lax.broadcasted_iota(jnp.int32, (128, 256), 1)
    ia, ib, ic = row >> 5, (row >> 3) & 3, row & 7
    for s in range(3):
        oz, oy, ox = offset_of(s, ia, ib, ic)
        src = ((z - oz) & 3) * 16 + ((y - oy) & 3) * 4 + ((x - ox) & 3)
        take = jnp.where((col == ia * 64 + src) & (ic < 4), 1.0, 0.0).astype(BF16)
        rows = jnp.dot(take, shifted, preferred_element_type=F32)
        isend[16 * s : 16 * s + 16] = rows.astype(BF16).reshape(16, 8, 128)
        irecv[16 * s] = rows[0:8].astype(BF16)
    gathered[0] = tokens[...]

    pl.semaphore_wait(barrier, near + 1)

    def send_rows(j, carry):
        a, b = j // 4, j % 4
        for s in range(3):
            remote(
                isend.at[16 * s + j], irecv.at[16 * s + j], i_send, i_recv,
                (peer(*offset_of(s, -a, -b, 0)), tp),
            ).start()
        return carry

    lax.fori_loop(1, 16, send_rows, 0)
    for c in (2, 1, 3):
        for s, (lo, width) in enumerate(SLICES):
            cols = pl.ds(lo, width)
            remote(
                tokens.at[:, cols], gathered.at[c, :, cols], g_send, g_recv,
                (peer(*offset_of(s, 0, 0, c)), tp),
            ).start()

    row = lax.broadcasted_iota(jnp.int32, (64, 64), 0)
    col = lax.broadcasted_iota(jnp.int32, (64, 64), 1)
    oy, ox = (row >> 2) & 3, row & 3
    oz = ((row >> 4) - oy - ox) & 3
    src = ((z - oz) & 3) * 16 + ((y - oy) & 3) * 4 + ((x - ox) & 3)
    ordered = jnp.dot(
        jnp.where(col == src, 1.0, 0.0), score[...], preferred_element_type=F32, precision=lax.Precision.HIGHEST
    )
    upright = ordered.T
    for o in range(64):
        scale[o * PICK : (o + 1) * PICK, :] = jnp.broadcast_to(upright[0:PICK, o : o + 1], (PICK, 128))

    remote(isend.at[0:45], irecv.at[0:45], i_send, i_recv, partner).wait_recv()
    token_row = lax.broadcasted_iota(jnp.int32, (TOK, 128), 0).astype(F32)

    def build(r, carry):
        for s in range(3):
            for c in range(4):
                total = jnp.zeros((8, 128), F32)
                for a in range(4):
                    b = (r - c - a + 8) % 4
                    total += irecv[16 * s + 4 * a + b].astype(F32)
                wanted = jnp.broadcast_to(total[c : c + 1] - 1.0, (TOK, 128))
                pick[(s * 4 + r) * 4 + c] = jnp.where(wanted == token_row, 1.0, 0.0).astype(BF16)
        return carry

    lax.fori_loop(0, 4, build, 0)
    remote(gathered.at[1:4], gathered.at[1:4], g_send, g_recv, partner).wait_recv()

    def dispatch(r, carry):
        for s, (lo, width) in enumerate(SLICES):
            for c in range(4):
                rows = lax.dot_general(
                    pick[(s * 4 + r) * 4 + c], gathered[c, :, lo : lo + width],
                    (((0,), (0,)), ((), ())), preferred_element_type=F32,
                ).astype(BF16)
                for a in range(4):
                    b = (r - c - a + 8) % 4
                    dsend[r * 16 + block_of(s, a, b, c), :, lo : lo + width] = rows[a * PICK : (a + 1) * PICK]
            mine = r * 16 + block_of(s, 0, 0, r)
            own[mine, :, lo : lo + width] = dsend[mine, :, lo : lo + width]

        def send(j, carry):
            a, b = j // 4, j % 4
            c = (r - a - b + 8) % 4
            for s, (lo, width) in enumerate(SLICES):
                blk = r * 16 + block_of(s, a, b, c)
                cols = pl.ds(lo, width)
                remote(
                    dsend.at[blk, :, cols], own.at[blk, :, cols], d_send, d_recv.at[r],
                    (peer(*offset_of(s, a, b, 0)), tp),
                ).start()
            return carry

        lax.fori_loop(1, 16, send, 0)
        return carry

    lax.fori_loop(0, 4, dispatch, 0)

    def forward(r):
        chunk = pl.ds(r * 16, 16)
        return remote(own.at[chunk], other.at[chunk], f_send, f_recv.at[r], partner)

    def pass_partial(r):
        return remote(psend.at[r], precv.at[r], p_send, p_recv.at[r], partner)

    def arrived(r):
        part = pl.ds(r * 16, 15)
        remote(own.at[part], own.at[part], d_send, d_recv.at[r], partner).wait_recv()

    def finish(r):
        pass_partial(r).wait_recv()
        factor = jnp.concatenate([scale[pl.ds(pl.multiple_of(r * ROWS, ROWS), ROWS), :]] * 2, axis=1)
        for n in range(4):
            cols = slice(n * 256, (n + 1) * 256)
            summed = pown[r, :, cols].astype(F32) + precv[r, :, cols].astype(F32)
            wt[pl.ds(r * 16, 16), :, cols] = (summed * factor).astype(BF16).reshape(16, PICK, 256)
        for s, (lo, width) in enumerate(SLICES):
            ret[r * 20, :, lo : lo + width] = wt[r * 16 + block_of(s, 0, 0, r), :, lo : lo + width]

        def send(j, carry):
            a, b = j // 4, j % 4
            c = (r - a - b + 8) % 4
            for s, (lo, width) in enumerate(SLICES):
                cols = pl.ds(lo, width)
                remote(
                    wt.at[r * 16 + block_of(s, a, b, c), :, cols], ret.at[r * 16 + c * 4 + a, :, cols],
                    r_send, r_recv.at[r], (peer(*offset_of(s, -a, -b, 0)), tp),
                ).start()
            return carry

        lax.fori_loop(1, 16, send, 0)

    for copy in weights:
        copy.wait()
    mine_at = pl.multiple_of(tp * HALF, HALF)
    other_at = pl.multiple_of((1 - tp) * HALF, HALF)

    def ffn(r, carry):
        arrived(r)
        forward(r).start()

        @pl.when(r > 0)
        def _():
            finish(r - 1)

        forward(r).wait_recv()
        x_own = own[pl.ds(r * 16, 16)].reshape(ROWS, HALF)
        x_other = other[pl.ds(r * 16, 16)].reshape(ROWS, HALF)
        for n in range(4):
            cols = slice(n * 256, (n + 1) * 256)
            gate = jnp.dot(x_own, wg[pl.ds(mine_at, HALF), cols], preferred_element_type=F32)
            gate += jnp.dot(x_other, wg[pl.ds(other_at, HALF), cols], preferred_element_type=F32)
            up = jnp.dot(x_own, wu[pl.ds(mine_at, HALF), cols], preferred_element_type=F32)
            up += jnp.dot(x_other, wu[pl.ds(other_at, HALF), cols], preferred_element_type=F32)
            hidden[:, cols] = (gate / (1.0 + jnp.exp(-gate)) * up).astype(BF16)
        for n in range(4):
            psend[r, :, n * 256 : (n + 1) * 256] = jnp.dot(
                hidden[...], wd[:, pl.ds(pl.multiple_of(other_at + n * 256, 256), 256)], preferred_element_type=F32
            ).astype(BF16)
        pass_partial(r).start()
        for n in range(4):
            pown[r, :, n * 256 : (n + 1) * 256] = jnp.dot(
                hidden[...], wd[:, pl.ds(pl.multiple_of(mine_at + n * 256, 256), 256)], preferred_element_type=F32
            ).astype(BF16)
        return carry

    lax.fori_loop(0, 4, ffn, 0)
    finish(3)

    sums[...] = jnp.zeros_like(sums)

    def combine(r, carry):
        part = pl.ds(r * 16, 15)
        remote(ret.at[part], ret.at[part], r_send, r_recv.at[r], partner).wait_recv()
        for s, (lo, width) in enumerate(SLICES):
            for c in range(4):
                rows = ret[pl.ds(r * 16 + c * 4, 4), :, lo : lo + width].reshape(4 * PICK, width)
                rows = jnp.concatenate([rows, jnp.zeros((128 - 4 * PICK, width), BF16)], axis=0)
                sums[c, :, lo : lo + width] += jnp.dot(
                    pick[(s * 4 + r) * 4 + c], rows, preferred_element_type=F32
                )
        return carry

    lax.fori_loop(0, 4, combine, 0)
    for c in (2, 1, 3):
        rsend[c - 1] = sums[c].astype(BF16)
        for s, (lo, width) in enumerate(SLICES):
            cols = pl.ds(lo, width)
            remote(
                rsend.at[c - 1, :, cols], rrecv.at[c - 1, :, cols], q_send, q_recv,
                (peer(*offset_of(s, 0, 0, -c)), tp),
            ).start()
    remote(rrecv.at[0:3], rrecv.at[0:3], q_send, q_recv, partner).wait_recv()
    total = sums[0]
    for c in range(3):
        total += rrecv[c].astype(F32)
    out[...] = total.astype(BF16)

    remote(isend.at[0:45], irecv.at[0:45], i_send, i_recv, partner).wait_send()
    remote(gathered.at[1:4], gathered.at[1:4], g_send, g_recv, partner).wait_send()
    remote(dsend.at[0:60], dsend.at[0:60], d_send, d_recv.at[0], partner).wait_send()
    remote(own, other, f_send, f_recv.at[0], partner).wait_send()
    remote(psend, precv, p_send, p_recv.at[0], partner).wait_send()
    remote(wt.at[0:60], ret.at[0:60], r_send, r_recv.at[0], partner).wait_send()
    remote(rsend, rrecv, q_send, q_recv, partner).wait_send()


def on_device(tokens, chosen, gate_score, gate_weight, up_weight, down_weight):
    vmem = pl.BlockSpec(memory_space=pltpu.VMEM)
    hbm = pl.BlockSpec(memory_space=pl.ANY)
    dma = pltpu.SemaphoreType.DMA
    chosen = jnp.pad(chosen.reshape(64, PICK), ((0, 0), (0, 128 - PICK)))
    score = jnp.pad(gate_score.reshape(64, PICK), ((0, 0), (0, 128 - PICK)))
    blocks = pltpu.VMEM((64, PICK, HALF), BF16)
    partial = pltpu.VMEM((4, ROWS, HALF), BF16)
    return pl.pallas_call(
        kernel,
        out_shape=jax.ShapeDtypeStruct((TOK, HALF), BF16),
        in_specs=[vmem, vmem, vmem, hbm, hbm, hbm],
        out_specs=vmem,
        scratch_shapes=[
            pltpu.VMEM((2048, 1024), BF16), pltpu.VMEM((2048, 1024), BF16), pltpu.VMEM((1024, 2048), BF16),
            pltpu.VMEM((4, TOK, HALF), BF16),
            pltpu.VMEM((48, 8, 128), BF16), pltpu.VMEM((48, 8, 128), BF16),
            pltpu.VMEM((48, TOK, 128), BF16),
            blocks, blocks, blocks,
            pltpu.VMEM((ROWS, 1024), BF16),
            partial, partial, partial,
            blocks, blocks,
            pltpu.VMEM((4, TOK, HALF), F32),
            pltpu.VMEM((3, TOK, HALF), BF16), pltpu.VMEM((3, TOK, HALF), BF16),
            pltpu.VMEM((64 * PICK, 128), F32),
            dma((3,)), dma, dma, dma, dma, dma, dma((4,)), dma, dma((4,)), dma, dma((4,)),
            dma, dma((4,)), dma, dma,
        ],
        compiler_params=pltpu.CompilerParams(
            collective_id=0, has_side_effects=True, vmem_limit_bytes=63 << 20
        ),
        cost_estimate=pl.CostEstimate(flops=20_000_000_000, bytes_accessed=14_000_000, transcendentals=1_600_000),
    )(tokens, chosen, score, gate_weight[0], up_weight[0], down_weight[0])


def solution(mesh):
    in_specs = (
        P("ep", "tp"),
        P("ep", None),
        P("ep", None),
        P("ep", None, "tp"),
        P("ep", None, "tp"),
        P("ep", "tp", None),
    )
    out_specs = P("ep", "tp")
    return jax.shard_map(
        on_device, mesh=mesh, in_specs=in_specs, out_specs=out_specs, check_vma=False
    )
```

```python
import jax
import jax.numpy as jnp
from jax import lax
from jax.experimental import pallas as pl
from jax.experimental.pallas import tpu as pltpu
from jax.sharding import PartitionSpec as P

BF16 = jnp.bfloat16
F32 = jnp.float32
MESH = pl.DeviceIdType.MESH
TOK = 192
PICK = 24
HALF = 1024
ROWS = 16 * PICK
CAP = 64 * PICK
SLICES = ((0, 384), (384, 384), (768, 256))


def offset_of(s, a, b, c):
    if s == 0:
        return c, a, b
    if s == 1:
        return a, c, b
    return a, b, c


def kernel(
    tokens, chosen, score, wg_hbm, wu_hbm, wd_hbm, out,
    wg, wu, wd, gathered, isend, passed, irecv, pick, dsend, own, other, gate_acc, up_acc, hidden, pown, psend, precv,
    wt, ret, sums, rsend, rrecv, scale,
    w_sem, i_send, i_recv, j_send, j_recv, g_send, g_recv, d_send, d_recv, f_send, f_recv, p_send, p_recv,
    r_send, r_recv, q_send, q_recv,
):
    ep = lax.axis_index("ep")
    tp = lax.axis_index("tp")
    z, y, x = ep // 16, (ep // 4) % 4, ep % 4
    u, v = y + tp * (x - y), x + tp * (y - x)
    u_step, v_step = 4 - 3 * tp, 1 + 3 * tp

    z_at = [lax.rem(z + k, 4) * 16 for k in range(4)]
    u_at = [lax.rem(u + k, 4) * u_step for k in range(4)]
    v_at = [lax.rem(v + k, 4) * v_step for k in range(4)]

    def peer(dz, du, dv):
        return z_at[dz % 4] + u_at[du % 4] + v_at[dv % 4]

    def remote(src, dst, send, recv, dev):
        return pltpu.make_async_remote_copy(
            src_ref=src, dst_ref=dst, send_sem=send, recv_sem=recv, device_id=dev, device_id_type=MESH
        )

    partner = (ep, 1 - tp)

    def block_of(s, a, b, c):
        dz, du, dv = offset_of(s, a, b, c)
        return du * u_step + dv * v_step

    weights = [
        pltpu.make_async_copy(src, dst, w_sem.at[i])
        for i, (src, dst) in enumerate(((wg_hbm, wg), (wu_hbm, wu), (wd_hbm, wd)))
    ]
    for copy in weights:
        copy.start()

    barrier = pltpu.get_barrier_semaphore()
    for s in range(3):
        for c in (2, 1, 3):
            pl.semaphore_signal(
                barrier, 1, device_id=(peer(*offset_of(s, 0, 0, c)), tp), device_id_type=MESH
            )
    pl.semaphore_signal(barrier, 1, device_id=partner, device_id_type=MESH)

    lane = lax.broadcasted_iota(jnp.int32, (1, CAP), 1)
    home = ((lane.astype(F32) + 0.5) * (1.0 / PICK)).astype(jnp.int32)
    local = (chosen[...] - TOK * home + 1).astype(F32)
    place = lax.broadcasted_iota(jnp.int32, (CAP, 128), 0)
    place -= PICK * ((place.astype(F32) + 0.5) * (1.0 / PICK)).astype(jnp.int32)
    place = lax.broadcasted_iota(jnp.int32, (CAP, 128), 1) - place
    row = lax.broadcasted_iota(jnp.int32, (32, CAP), 0)
    ib, ic = row >> 3, row & 7
    homes = jnp.broadcast_to(home, (32, CAP))
    locals_ = jnp.broadcast_to(local, (32, CAP))
    for a in range(4):
        spread = jnp.where(place == a * PICK, 1.0, 0.0).astype(BF16)
        for s in range(3):
            oz, ou, ov = offset_of(s, a, ib, ic)
            src = ((z - oz) & 3) * 16 + ((u - ou) & 3) * u_step + ((v - ov) & 3) * v_step
            src = jnp.where(ic < 4, src, -1)
            take = jnp.where(homes == src, locals_, 0.0).astype(BF16)
            rows = jnp.dot(take, spread, preferred_element_type=F32).astype(BF16)
            isend[s, a] = rows.reshape(4, 8, 128)
            if a == 0:
                passed[s, :, 0] = rows.reshape(4, 8, 128)
    gathered[0] = tokens[...]

    pl.semaphore_wait(barrier, 10)

    for s in range(3):
        for a in (2, 1, 3):
            remote(
                isend.at[s, a], passed.at[s, :, a], i_send, i_recv, (peer(*offset_of(s, -a, 0, 0)), tp)
            ).start()

    def gather(c, lines):
        for s, (lo, width) in enumerate(SLICES):
            cols = pl.ds(lo, width)
            remote(
                tokens.at[lines, cols], gathered.at[c, lines, cols], g_send, g_recv,
                (peer(*offset_of(s, 0, 0, c)), tp),
            ).start()

    gather(1, pl.ds(0, 128))
    gather(3, pl.ds(0, 128))
    remote(passed.at[:, :, 0:3], passed.at[:, :, 1:4], i_send, i_recv, partner).wait_recv()
    for s in range(3):
        for b in (2, 1, 3):
            remote(
                passed.at[s, b], irecv.at[s, b], j_send, j_recv, (peer(*offset_of(s, 0, -b, 0)), tp)
            ).start()
        irecv[s, 0] = passed[s, 0]
    gather(1, pl.ds(128, 64))
    gather(3, pl.ds(128, 64))
    gather(2, pl.ds(0, TOK))

    row = lax.broadcasted_iota(jnp.int32, (64, CAP), 0)
    oy, ox = (row >> 2) & 3, row & 3
    oz = ((row >> 4) - oy - ox) & 3
    src = ((z - oz) & 3) * 16 + ((y - oy) & 3) * 4 + ((x - ox) & 3)
    left = jnp.where(jnp.broadcast_to(home, (64, CAP)) == src, jnp.broadcast_to(score[...], (64, CAP)), 0.0)
    spread = jnp.where(place == 0, 1.0, 0.0).astype(BF16)
    ordered = jnp.zeros((64, 128), F32)
    for _ in range(3):
        term = left.astype(BF16)
        ordered += jnp.dot(term, spread, preferred_element_type=F32)
        left -= term.astype(F32)
    upright = ordered.T
    for o in range(64):
        scale[o * PICK : (o + 1) * PICK, :] = jnp.broadcast_to(upright[0:PICK, o : o + 1], (PICK, 128))

    remote(irecv.at[:, 0:3], irecv.at[:, 1:4], j_send, j_recv, partner).wait_recv()
    token_row = lax.broadcasted_iota(jnp.int32, (TOK, 128), 0).astype(F32)

    def dispatch(r, c):
        for s, (lo, width) in enumerate(SLICES):
            cols = pl.ds(lo, width)
            total = irecv[s, (r - c) % 4, 0].astype(F32)
            for a in range(1, 4):
                total += irecv[s, (r - c - a) % 4, a].astype(F32)
            wanted = jnp.broadcast_to(total[c : c + 1] - 1.0, (TOK, 128))
            chosen_rows = jnp.where(wanted == token_row, 1.0, 0.0).astype(BF16)
            pick[(s * 4 + r) * 4 + c] = chosen_rows
            rows = lax.dot_general(
                chosen_rows, gathered[c, :, lo : lo + width],
                (((0,), (0,)), ((), ())), preferred_element_type=F32,
            ).astype(BF16)
            for a in range(4):
                b = (r - c - a) % 4
                blk = r * 16 + block_of(s, a, b, c)
                if a == 0 and b == 0:
                    own[blk, :, lo : lo + width] = rows[0:PICK]
                    continue
                dsend[blk, :, lo : lo + width] = rows[a * PICK : (a + 1) * PICK]
                remote(
                    dsend.at[blk, :, cols], own.at[blk, :, cols], d_send, d_recv.at[r],
                    (peer(*offset_of(s, a, b, 0)), tp),
                ).start()

    dispatch(0, 0)
    dispatch(1, 0)
    remote(gathered.at[0:3], gathered.at[1:4], g_send, g_recv, partner).wait_recv()
    for r in range(4):
        for c in (0, 1, 3, 2):
            if c or r > 1:
                dispatch(r, c)

    def forward(r):
        chunk = pl.ds(r * 16, 16)
        return remote(own.at[chunk], other.at[chunk], f_send, f_recv.at[r], partner)

    def pass_partial(r, half):
        return remote(psend.at[r, half], precv.at[r, half], p_send, p_recv.at[r, half], partner)

    def arrived(r):
        part = pl.ds(r * 16, 15)
        remote(own.at[part], own.at[part], d_send, d_recv.at[r], partner).wait_recv()

    def finish(r):
        back = [lax.rem(r + 4 - k, 4) for k in range(4)]
        first = pl.multiple_of(r * ROWS, ROWS)
        factor = jnp.concatenate([scale[pl.ds(first, ROWS), :]] * 4, axis=1)
        for half in range(2):
            pass_partial(r, half).wait_recv()
            summed = pown[r, half].astype(F32) + precv[r, half].astype(F32)
            wt[pl.ds(r * 16, 16), :, half * 512 : half * 512 + 512] = (
                (summed * factor).astype(BF16).reshape(16, PICK, 512)
            )
            for s, (lo, width) in enumerate(SLICES):
                if (lo + width > 512) != (half == 1):
                    continue
                cols = pl.ds(lo, width)
                ret[r * 20, :, lo : lo + width] = wt[r * 16 + block_of(s, 0, 0, r), :, lo : lo + width]
                for j in range(1, 16):
                    a, b = j // 4, j % 4
                    c = back[(a + b) % 4]
                    remote(
                        wt.at[r * 16 + block_of(s, a, b, c), :, cols], ret.at[r * 16 + c * 4 + a, :, cols],
                        r_send, r_recv.at[r, s], (peer(*offset_of(s, -a, -b, 0)), tp),
                    ).start()

    for copy in weights:
        copy.wait()
    mine_at = pl.multiple_of(tp * HALF, HALF)
    other_at = pl.multiple_of((1 - tp) * HALF, HALF)

    def ffn(r, carry):
        arrived(r)
        forward(r).start()
        x_own = own[pl.ds(r * 16, 16)].reshape(ROWS, HALF)
        for n in range(4):
            cols = slice(n * 256, (n + 1) * 256)
            gate_acc[:, cols] = jnp.dot(x_own, wg[pl.ds(mine_at, HALF), cols], preferred_element_type=F32)

        @pl.when(r > 0)
        def _():
            finish(r - 1)

        for n in range(4):
            cols = slice(n * 256, (n + 1) * 256)
            up_acc[:, cols] = jnp.dot(x_own, wu[pl.ds(mine_at, HALF), cols], preferred_element_type=F32)
        forward(r).wait_recv()
        x_other = other[pl.ds(r * 16, 16)].reshape(ROWS, HALF)
        for n in range(4):
            cols = slice(n * 256, (n + 1) * 256)
            gate = gate_acc[:, cols] + jnp.dot(
                x_other, wg[pl.ds(other_at, HALF), cols], preferred_element_type=F32
            )
            up = up_acc[:, cols] + jnp.dot(x_other, wu[pl.ds(other_at, HALF), cols], preferred_element_type=F32)
            hidden[:, cols] = (gate / (1.0 + jnp.exp(-gate)) * up).astype(BF16)
        for half in range(2):
            for n in range(2):
                at = pl.multiple_of(other_at + half * 512 + n * 256, 256)
                psend[r, half, :, n * 256 : n * 256 + 256] = jnp.dot(
                    hidden[...], wd[:, pl.ds(at, 256)], preferred_element_type=F32
                ).astype(BF16)
            pass_partial(r, half).start()
        for half in range(2):
            for n in range(2):
                at = pl.multiple_of(mine_at + half * 512 + n * 256, 256)
                pown[r, half, :, n * 256 : n * 256 + 256] = jnp.dot(
                    hidden[...], wd[:, pl.ds(at, 256)], preferred_element_type=F32
                ).astype(BF16)
        return carry

    lax.fori_loop(0, 4, ffn, 0)
    finish(3)

    sums[...] = jnp.zeros_like(sums)

    def combine(r, s):
        lo, width = SLICES[s]
        part = ret.at[pl.ds(r * 16, 15), :, pl.ds(lo, width)]
        remote(part, part, r_send, r_recv.at[r, s], partner).wait_recv()
        for c in range(4):
            rows = ret[pl.ds(r * 16 + c * 4, 4), :, lo : lo + width].reshape(4 * PICK, width)
            rows = jnp.concatenate([rows, jnp.zeros((128 - 4 * PICK, width), BF16)], axis=0)
            sums[c, :, lo : lo + width] += jnp.dot(
                pick[(s * 4 + r) * 4 + c], rows, preferred_element_type=F32
            )

    def combine_all(r, carry):
        for s in range(3):
            combine(r, s)
        return carry

    lax.fori_loop(0, 3, combine_all, 0)
    for s, (lo, width) in enumerate(SLICES):
        combine(3, s)
        cols = pl.ds(lo, width)
        for c in (2, 1, 3):
            rsend[c - 1, :, lo : lo + width] = sums[c, :, lo : lo + width].astype(BF16)
            remote(
                rsend.at[c - 1, :, cols], rrecv.at[c - 1, :, cols], q_send, q_recv.at[s],
                (peer(*offset_of(s, 0, 0, -c)), tp),
            ).start()
    for s, (lo, width) in enumerate(SLICES):
        part = rrecv.at[:, :, pl.ds(lo, width)]
        remote(part, part, q_send, q_recv.at[s], partner).wait_recv()
        total = sums[0, :, lo : lo + width]
        for c in range(3):
            total += rrecv[c, :, lo : lo + width].astype(F32)
        out[:, lo : lo + width] = total.astype(BF16)

    remote(passed.at[:, :, 0:3], passed.at[:, :, 1:4], i_send, i_recv, partner).wait_send()
    remote(irecv.at[:, 0:3], irecv.at[:, 1:4], j_send, j_recv, partner).wait_send()
    remote(gathered.at[0:3], gathered.at[1:4], g_send, g_recv, partner).wait_send()
    remote(dsend.at[0:60], dsend.at[0:60], d_send, d_recv.at[0], partner).wait_send()
    remote(own, other, f_send, f_recv.at[0], partner).wait_send()
    remote(psend, precv, p_send, p_recv.at[0, 0], partner).wait_send()
    remote(wt.at[0:60], ret.at[0:60], r_send, r_recv.at[0, 0], partner).wait_send()
    remote(rsend, rrecv, q_send, q_recv.at[0], partner).wait_send()


def on_device(tokens, chosen, gate_score, gate_weight, up_weight, down_weight):
    vmem = pl.BlockSpec(memory_space=pltpu.VMEM)
    hbm = pl.BlockSpec(memory_space=pl.ANY)
    dma = pltpu.SemaphoreType.DMA
    blocks = pltpu.VMEM((64, PICK, HALF), BF16)
    partial = pltpu.VMEM((4, 2, ROWS, 512), BF16)
    tiles = pltpu.VMEM((3, 4, 4, 8, 128), BF16)
    return pl.pallas_call(
        kernel,
        out_shape=jax.ShapeDtypeStruct((TOK, HALF), BF16),
        in_specs=[vmem, vmem, vmem, hbm, hbm, hbm],
        out_specs=vmem,
        scratch_shapes=[
            pltpu.VMEM((2048, 1024), BF16), pltpu.VMEM((2048, 1024), BF16), pltpu.VMEM((1024, 2048), BF16),
            pltpu.VMEM((4, TOK, HALF), BF16),
            tiles, tiles, tiles,
            pltpu.VMEM((48, TOK, 128), BF16),
            blocks, blocks, blocks,
            pltpu.VMEM((ROWS, 1024), F32), pltpu.VMEM((ROWS, 1024), F32), pltpu.VMEM((ROWS, 1024), BF16),
            partial, partial, partial,
            blocks, blocks,
            pltpu.VMEM((4, TOK, HALF), F32),
            pltpu.VMEM((3, TOK, HALF), BF16), pltpu.VMEM((3, TOK, HALF), BF16),
            pltpu.VMEM((64 * PICK, 128), F32),
            dma((3,)), dma, dma, dma, dma, dma, dma, dma, dma((4,)), dma, dma((4,)), dma, dma((4, 2)),
            dma, dma((4, 3)), dma, dma((3,)),
        ],
        compiler_params=pltpu.CompilerParams(
            collective_id=0, has_side_effects=True, vmem_limit_bytes=63 << 20
        ),
        cost_estimate=pl.CostEstimate(flops=20_000_000_000, bytes_accessed=14_000_000, transcendentals=1_600_000),
    )(tokens, chosen, gate_score, gate_weight[0], up_weight[0], down_weight[0])


def solution(mesh):
    in_specs = (
        P("ep", "tp"),
        P("ep", None),
        P("ep", None),
        P("ep", None, "tp"),
        P("ep", None, "tp"),
        P("ep", "tp", None),
    )
    out_specs = P("ep", "tp")
    return jax.shard_map(
        on_device, mesh=mesh, in_specs=in_specs, out_specs=out_specs, check_vma=False
    )
```

```python
import jax
import jax.numpy as jnp
from jax import lax
from jax.experimental import pallas as pl
from jax.experimental.pallas import tpu as pltpu
from jax.sharding import PartitionSpec as P

BF16 = jnp.bfloat16
F32 = jnp.float32
MESH = pl.DeviceIdType.MESH
TOK = 192
PICK = 24
HALF = 1024
CAP = 64 * PICK
PART = 8 * PICK
SLICES = ((0, 384), (384, 384), (768, 256))


def offset_of(s, a, b, c):
    if s == 0:
        return c, a, b
    if s == 1:
        return a, c, b
    return a, b, c


def kernel(
    tokens, chosen, score, wg_hbm, wu_hbm, wd_hbm, out,
    wg, wu, wd, gathered, isend, passed, irecv, pick, dsend, own, other, gate_acc, up_acc, hidden, pown, psend, precv,
    wt, ret, sums, rsend, rrecv, scale,
    w_sem, i_send, i_recv, j_send, j_recv, g_send, g_recv, d_send, d_recv, f_send, f_recv, p_send, p_recv,
    r_send, r_recv, q_send, q_recv,
):
    ep = lax.axis_index("ep")
    tp = lax.axis_index("tp")
    z, y, x = ep // 16, (ep // 4) % 4, ep % 4
    u, v = y + tp * (x - y), x + tp * (y - x)
    u_step, v_step = 4 - 3 * tp, 1 + 3 * tp

    z_at = [lax.rem(z + k, 4) * 16 for k in range(4)]
    u_at = [lax.rem(u + k, 4) * u_step for k in range(4)]
    v_at = [lax.rem(v + k, 4) * v_step for k in range(4)]

    def peer(dz, du, dv):
        return z_at[dz % 4] + u_at[du % 4] + v_at[dv % 4]

    def remote(src, dst, send, recv, dev):
        return pltpu.make_async_remote_copy(
            src_ref=src, dst_ref=dst, send_sem=send, recv_sem=recv, device_id=dev, device_id_type=MESH
        )

    partner = (ep, 1 - tp)

    def half_of(s, a, b, c):
        _, du, dv = offset_of(s, a, b, c)
        return (du // 2 + dv // 2) % 2

    def block_of(s, a, b, c):
        _, du, dv = offset_of(s, a, b, c)
        on_0, on_1 = du * 2 + dv % 2, dv * 2 + du % 2
        return half_of(s, a, b, c) * 8 + on_0 + tp * (on_1 - on_0)

    weights = [
        pltpu.make_async_copy(src, dst, w_sem.at[i])
        for i, (src, dst) in enumerate(((wg_hbm, wg), (wu_hbm, wu), (wd_hbm, wd)))
    ]
    for copy in weights:
        copy.start()

    barrier = pltpu.get_barrier_semaphore()
    for s in range(3):
        for c in (2, 1, 3):
            pl.semaphore_signal(
                barrier, 1, device_id=(peer(*offset_of(s, 0, 0, c)), tp), device_id_type=MESH
            )
    pl.semaphore_signal(barrier, 1, device_id=partner, device_id_type=MESH)

    lane = lax.broadcasted_iota(jnp.int32, (1, CAP), 1)
    home = ((lane.astype(F32) + 0.5) * (1.0 / PICK)).astype(jnp.int32)
    local = (chosen[...] - TOK * home + 1).astype(F32)
    place = lax.broadcasted_iota(jnp.int32, (CAP, 128), 0)
    place -= PICK * ((place.astype(F32) + 0.5) * (1.0 / PICK)).astype(jnp.int32)
    place = lax.broadcasted_iota(jnp.int32, (CAP, 128), 1) - place
    row = lax.broadcasted_iota(jnp.int32, (32, CAP), 0)
    ib, ic = row >> 3, row & 7
    homes = jnp.broadcast_to(home, (32, CAP))
    locals_ = jnp.broadcast_to(local, (32, CAP))
    for a in range(4):
        spread = jnp.where(place == a * PICK, 1.0, 0.0).astype(BF16)
        for s in range(3):
            oz, ou, ov = offset_of(s, a, ib, ic)
            src = ((z - oz) & 3) * 16 + ((u - ou) & 3) * u_step + ((v - ov) & 3) * v_step
            src = jnp.where(ic < 4, src, -1)
            take = jnp.where(homes == src, locals_, 0.0).astype(BF16)
            rows = jnp.dot(take, spread, preferred_element_type=F32).astype(BF16)
            isend[s, a] = rows.reshape(4, 8, 128)
            if a == 0:
                passed[s, :, 0] = rows.reshape(4, 8, 128)
    gathered[0] = tokens[...]

    pl.semaphore_wait(barrier, 10)

    for s in range(3):
        for a in (2, 1, 3):
            remote(
                isend.at[s, a], passed.at[s, :, a], i_send, i_recv, (peer(*offset_of(s, -a, 0, 0)), tp)
            ).start()

    def gather(c, lines):
        for s, (lo, width) in enumerate(SLICES):
            cols = pl.ds(lo, width)
            remote(
                tokens.at[lines, cols], gathered.at[c, lines, cols], g_send, g_recv,
                (peer(*offset_of(s, 0, 0, c)), tp),
            ).start()

    gather(1, pl.ds(0, 128))
    gather(3, pl.ds(0, 128))
    remote(passed.at[:, :, 0:3], passed.at[:, :, 1:4], i_send, i_recv, partner).wait_recv()
    for s in range(3):
        for b in (2, 1, 3):
            remote(
                passed.at[s, b], irecv.at[s, b], j_send, j_recv, (peer(*offset_of(s, 0, -b, 0)), tp)
            ).start()
        irecv[s, 0] = passed[s, 0]
    gather(1, pl.ds(128, 64))
    gather(3, pl.ds(128, 64))
    gather(2, pl.ds(0, TOK))

    row = lax.broadcasted_iota(jnp.int32, (64, CAP), 0)
    oy = (row >> 1) & 3
    ox = 2 * (((oy >> 1) + (row >> 3)) & 1) + (row & 1)
    oz = ((row >> 4) - oy - ox) & 3
    src = ((z - oz) & 3) * 16 + ((y - oy) & 3) * 4 + ((x - ox) & 3)
    left = jnp.where(jnp.broadcast_to(home, (64, CAP)) == src, jnp.broadcast_to(score[...], (64, CAP)), 0.0)
    spread = jnp.where(place == 0, 1.0, 0.0).astype(BF16)
    ordered = jnp.zeros((64, 128), F32)
    for _ in range(3):
        term = left.astype(BF16)
        ordered += jnp.dot(term, spread, preferred_element_type=F32)
        left -= term.astype(F32)
    upright = ordered.T
    for o in range(64):
        scale[o * PICK : (o + 1) * PICK, :] = jnp.broadcast_to(upright[0:PICK, o : o + 1], (PICK, 128))

    remote(irecv.at[:, 0:3], irecv.at[:, 1:4], j_send, j_recv, partner).wait_recv()
    token_row = lax.broadcasted_iota(jnp.int32, (TOK, 128), 0).astype(F32)

    def dispatch(r, c):
        for s, (lo, width) in enumerate(SLICES):
            cols = pl.ds(lo, width)
            total = irecv[s, (r - c) % 4, 0].astype(F32)
            for a in range(1, 4):
                total += irecv[s, (r - c - a) % 4, a].astype(F32)
            wanted = jnp.broadcast_to(total[c : c + 1] - 1.0, (TOK, 128))
            chosen_rows = jnp.where(wanted == token_row, 1.0, 0.0).astype(BF16)
            pick[(s * 4 + r) * 4 + c] = chosen_rows
            rows = lax.dot_general(
                chosen_rows, gathered[c, :, lo : lo + width],
                (((0,), (0,)), ((), ())), preferred_element_type=F32,
            ).astype(BF16)
            for a in range(4):
                b = (r - c - a) % 4
                blk = r * 16 + block_of(s, a, b, c)
                if a == 0 and b == 0:
                    own[blk, :, lo : lo + width] = rows[0:PICK]
                else:
                    dsend[blk, :, lo : lo + width] = rows[a * PICK : (a + 1) * PICK]

    def send_out(r, directions):
        for half in range(2):
            for c in directions:
                for a in range(4):
                    for s, (lo, width) in enumerate(SLICES):
                        b = (r - c - a) % 4
                        if (a == 0 and b == 0) or half_of(s, a, b, c) != half:
                            continue
                        blk, cols = r * 16 + block_of(s, a, b, c), pl.ds(lo, width)
                        remote(
                            dsend.at[blk, :, cols], own.at[blk, :, cols], d_send, d_recv.at[2 * r + half, s],
                            (peer(*offset_of(s, a, b, 0)), tp),
                        ).start()

    for r in range(2):
        dispatch(r, 0)
        send_out(r, (0,))
    remote(gathered.at[0:3], gathered.at[1:4], g_send, g_recv, partner).wait_recv()
    for r in range(4):
        rest = (1, 3, 2) if r < 2 else (0, 1, 3, 2)
        for c in rest:
            dispatch(r, c)
        send_out(r, rest)

    def forward(k):
        part = pl.ds(k * 8, 8)
        return remote(own.at[part], other.at[part], f_send, f_recv.at[k], partner)

    def pass_partial(k):
        return remote(psend.at[k], precv.at[k], p_send, p_recv.at[k], partner)

    def arrived(k):
        r, half = k // 2, k % 2
        for s, (lo, width) in enumerate(SLICES):
            count = 8 - (half_of(s, 0, 0, r) == half)
            part = own.at[pl.ds(k * 8, count), :, pl.ds(lo, width)]
            remote(part, part, d_send, d_recv.at[k, s], partner).wait_recv()

    def finish(k):
        r, half = k // 2, k % 2
        pass_partial(k).wait_recv()
        factor = jnp.concatenate([scale[k * PART : (k + 1) * PART, :]] * 4, axis=1)
        for n in range(2):
            cols = slice(n * 512, n * 512 + 512)
            summed = pown[k, :, cols].astype(F32) + precv[k, :, cols].astype(F32)
            wt[k * 8 : k * 8 + 8, :, cols] = (summed * factor).astype(BF16).reshape(8, PICK, 512)
        for s, (lo, width) in enumerate(SLICES):
            cols = pl.ds(lo, width)
            for a in range(4):
                for b in range(4):
                    c = (r - a - b) % 4
                    if half_of(s, a, b, c) != half:
                        continue
                    blk, place = r * 16 + block_of(s, a, b, c), r * 16 + c * 4 + a
                    if a == 0 and b == 0:
                        ret[place, :, lo : lo + width] = wt[blk, :, lo : lo + width]
                        continue
                    remote(
                        wt.at[blk, :, cols], ret.at[place, :, cols], r_send, r_recv.at[r, s],
                        (peer(*offset_of(s, -a, -b, 0)), tp),
                    ).start()

    for copy in weights:
        copy.wait()
    mine_at = pl.multiple_of(tp * HALF, HALF)
    other_at = pl.multiple_of((1 - tp) * HALF, HALF)

    tiles_of = [slice(n * 256, (n + 1) * 256) for n in range(4)]

    def up_own(k):
        rows = own[k * 8 : k * 8 + 8].reshape(PART, HALF)
        for cols in tiles_of:
            gate_acc[:, cols] = jnp.dot(rows, wg[pl.ds(mine_at, HALF), cols], preferred_element_type=F32)
            up_acc[:, cols] = jnp.dot(rows, wu[pl.ds(mine_at, HALF), cols], preferred_element_type=F32)

    def up_other(k):
        rows = other[k * 8 : k * 8 + 8].reshape(PART, HALF)
        for cols in tiles_of:
            gate = gate_acc[:, cols] + jnp.dot(rows, wg[pl.ds(other_at, HALF), cols], preferred_element_type=F32)
            up = up_acc[:, cols] + jnp.dot(rows, wu[pl.ds(other_at, HALF), cols], preferred_element_type=F32)
            hidden[:, cols] = (gate / (1.0 + jnp.exp(-gate)) * up).astype(BF16)

    def down(k):
        for n, cols in enumerate(tiles_of):
            at = pl.multiple_of(other_at + n * 256, 256)
            psend[k, :, cols] = jnp.dot(
                hidden[...], wd[:, pl.ds(at, 256)], preferred_element_type=F32
            ).astype(BF16)
        pass_partial(k).start()
        for n, cols in enumerate(tiles_of):
            at = pl.multiple_of(mine_at + n * 256, 256)
            pown[k, :, cols] = jnp.dot(
                hidden[...], wd[:, pl.ds(at, 256)], preferred_element_type=F32
            ).astype(BF16)

    for k in range(8):
        arrived(k)
        forward(k).start()
        up_own(k)
        if k:
            down(k - 1)
        forward(k).wait_recv()
        up_other(k)
        if k:
            finish(k - 1)
    down(7)
    finish(7)

    sums[...] = jnp.zeros_like(sums)

    def combine(r, s):
        lo, width = SLICES[s]
        part = ret.at[pl.ds(r * 16, 15), :, pl.ds(lo, width)]
        remote(part, part, r_send, r_recv.at[r, s], partner).wait_recv()
        for c in range(4):
            rows = ret[pl.ds(r * 16 + c * 4, 4), :, lo : lo + width].reshape(4 * PICK, width)
            rows = jnp.concatenate([rows, jnp.zeros((128 - 4 * PICK, width), BF16)], axis=0)
            sums[c, :, lo : lo + width] += jnp.dot(
                pick[(s * 4 + r) * 4 + c], rows, preferred_element_type=F32
            )

    def combine_all(r, carry):
        for s in range(3):
            combine(r, s)
        return carry

    lax.fori_loop(0, 3, combine_all, 0)
    for s, (lo, width) in enumerate(SLICES):
        combine(3, s)
        cols = pl.ds(lo, width)
        for c in (2, 1, 3):
            rsend[c - 1, :, lo : lo + width] = sums[c, :, lo : lo + width].astype(BF16)
            remote(
                rsend.at[c - 1, :, cols], rrecv.at[c - 1, :, cols], q_send, q_recv.at[s],
                (peer(*offset_of(s, 0, 0, -c)), tp),
            ).start()
    for s, (lo, width) in enumerate(SLICES):
        part = rrecv.at[:, :, pl.ds(lo, width)]
        remote(part, part, q_send, q_recv.at[s], partner).wait_recv()
        total = sums[0, :, lo : lo + width]
        for c in range(3):
            total += rrecv[c, :, lo : lo + width].astype(F32)
        out[:, lo : lo + width] = total.astype(BF16)

    remote(passed.at[:, :, 0:3], passed.at[:, :, 1:4], i_send, i_recv, partner).wait_send()
    remote(irecv.at[:, 0:3], irecv.at[:, 1:4], j_send, j_recv, partner).wait_send()
    remote(gathered.at[0:3], gathered.at[1:4], g_send, g_recv, partner).wait_send()
    remote(dsend.at[0:60], dsend.at[0:60], d_send, d_recv.at[0, 0], partner).wait_send()
    remote(own, other, f_send, f_recv.at[0], partner).wait_send()
    remote(psend, precv, p_send, p_recv.at[0], partner).wait_send()
    remote(wt.at[0:60], ret.at[0:60], r_send, r_recv.at[0, 0], partner).wait_send()
    remote(rsend, rrecv, q_send, q_recv.at[0], partner).wait_send()


def on_device(tokens, chosen, gate_score, gate_weight, up_weight, down_weight):
    vmem = pl.BlockSpec(memory_space=pltpu.VMEM)
    hbm = pl.BlockSpec(memory_space=pl.ANY)
    dma = pltpu.SemaphoreType.DMA
    blocks = pltpu.VMEM((64, PICK, HALF), BF16)
    partial = pltpu.VMEM((8, PART, HALF), BF16)
    tiles = pltpu.VMEM((3, 4, 4, 8, 128), BF16)
    return pl.pallas_call(
        kernel,
        out_shape=jax.ShapeDtypeStruct((TOK, HALF), BF16),
        in_specs=[vmem, vmem, vmem, hbm, hbm, hbm],
        out_specs=vmem,
        scratch_shapes=[
            pltpu.VMEM((2048, 1024), BF16), pltpu.VMEM((2048, 1024), BF16), pltpu.VMEM((1024, 2048), BF16),
            pltpu.VMEM((4, TOK, HALF), BF16),
            tiles, tiles, tiles,
            pltpu.VMEM((48, TOK, 128), BF16),
            blocks, blocks, blocks,
            pltpu.VMEM((PART, 1024), F32), pltpu.VMEM((PART, 1024), F32), pltpu.VMEM((PART, 1024), BF16),
            partial, partial, partial,
            blocks, blocks,
            pltpu.VMEM((4, TOK, HALF), F32),
            pltpu.VMEM((3, TOK, HALF), BF16), pltpu.VMEM((3, TOK, HALF), BF16),
            pltpu.VMEM((64 * PICK, 128), F32),
            dma((3,)), dma, dma, dma, dma, dma, dma, dma, dma((8, 3)), dma, dma((8,)), dma, dma((8,)),
            dma, dma((4, 3)), dma, dma((3,)),
        ],
        compiler_params=pltpu.CompilerParams(
            collective_id=0, has_side_effects=True, vmem_limit_bytes=63 << 20
        ),
        cost_estimate=pl.CostEstimate(flops=20_000_000_000, bytes_accessed=14_000_000, transcendentals=1_600_000),
    )(tokens, chosen, gate_score, gate_weight[0], up_weight[0], down_weight[0])


def solution(mesh):
    in_specs = (
        P("ep", "tp"),
        P("ep", None),
        P("ep", None),
        P("ep", None, "tp"),
        P("ep", None, "tp"),
        P("ep", "tp", None),
    )
    out_specs = P("ep", "tp")
    return jax.shard_map(
        on_device, mesh=mesh, in_specs=in_specs, out_specs=out_specs, check_vma=False
    )
```

```python
import jax
import jax.numpy as jnp
from jax import lax
from jax.experimental import pallas as pl
from jax.experimental.pallas import tpu as pltpu
from jax.sharding import PartitionSpec as P

BF16 = jnp.bfloat16
F32 = jnp.float32
MESH = pl.DeviceIdType.MESH
TOK = 192
PICK = 24
HALF = 1024
CAP = 64 * PICK
PART = 8 * PICK
SLICES = ((0, 384), (384, 384), (768, 256))


def offset_of(s, a, b, c):
    if s == 0:
        return c, a, b
    if s == 1:
        return a, c, b
    return a, b, c


def kernel(
    tokens, chosen, score, wg_hbm, wu_hbm, wd_hbm, out,
    wg, wu, wd, gathered, isend, passed, irecv, pick, dsend, own, other, gate_acc, up_acc, hidden, pown, psend, precv,
    wt, ret, sums, rsend, rrecv, scale,
    w_sem, i_send, i_recv, j_send, j_recv, g_send, g_recv, d_send, d_recv, f_send, f_recv, p_send, p_recv,
    r_send, r_recv, q_send, q_recv,
):
    ep = lax.axis_index("ep")
    tp = lax.axis_index("tp")
    z, y, x = ep // 16, (ep // 4) % 4, ep % 4
    u, v = y + tp * (x - y), x + tp * (y - x)
    u_step, v_step = 4 - 3 * tp, 1 + 3 * tp

    z_at = [lax.rem(z + k, 4) * 16 for k in range(4)]
    u_at = [lax.rem(u + k, 4) * u_step for k in range(4)]
    v_at = [lax.rem(v + k, 4) * v_step for k in range(4)]

    def peer(dz, du, dv):
        return z_at[dz % 4] + u_at[du % 4] + v_at[dv % 4]

    def remote(src, dst, send, recv, dev):
        return pltpu.make_async_remote_copy(
            src_ref=src, dst_ref=dst, send_sem=send, recv_sem=recv, device_id=dev, device_id_type=MESH
        )

    partner = (ep, 1 - tp)

    def half_of(s, a, b, c):
        _, du, dv = offset_of(s, a, b, c)
        return (du // 2 + dv // 2) % 2

    def block_of(s, a, b, c):
        _, du, dv = offset_of(s, a, b, c)
        on_0, on_1 = du * 2 + dv % 2, dv * 2 + du % 2
        return half_of(s, a, b, c) * 8 + on_0 + tp * (on_1 - on_0)

    weights = [
        pltpu.make_async_copy(src, dst, w_sem.at[i])
        for i, (src, dst) in enumerate(((wg_hbm, wg), (wu_hbm, wu), (wd_hbm, wd)))
    ]
    for copy in weights:
        copy.start()

    barrier = pltpu.get_barrier_semaphore()
    for s in range(3):
        for c in (2, 1, 3):
            pl.semaphore_signal(
                barrier, 1, device_id=(peer(*offset_of(s, 0, 0, c)), tp), device_id_type=MESH
            )
    pl.semaphore_signal(barrier, 1, device_id=partner, device_id_type=MESH)

    lane = lax.broadcasted_iota(jnp.int32, (1, CAP), 1)
    home = ((lane.astype(F32) + 0.5) * (1.0 / PICK)).astype(jnp.int32)
    local = (chosen[...] - TOK * home + 1).astype(F32)
    place = lax.broadcasted_iota(jnp.int32, (CAP, 128), 0)
    place -= PICK * ((place.astype(F32) + 0.5) * (1.0 / PICK)).astype(jnp.int32)
    place = lax.broadcasted_iota(jnp.int32, (CAP, 128), 1) - place
    row = lax.broadcasted_iota(jnp.int32, (128, 128), 0)
    ia, ib, ic = row >> 5, (row >> 3) & 3, row & 7
    homes = jnp.broadcast_to(home, (128, CAP))
    locals_ = jnp.broadcast_to(local, (128, CAP))
    takes = []
    for s in range(3):
        oz, ou, ov = offset_of(s, ia, ib, ic)
        src = ((z - oz) & 3) * 16 + ((u - ou) & 3) * u_step + ((v - ov) & 3) * v_step
        src = jnp.concatenate([jnp.where(ic < 4, src, -1)] * (CAP // 128), axis=1)
        takes.append(jnp.where(homes == src, locals_, 0.0).astype(BF16))
    spread = jnp.where(place == 0, 1.0, 0.0).astype(BF16)
    rows = jnp.dot(jnp.concatenate(takes, axis=0), spread, preferred_element_type=F32)
    for s in range(3):
        for a in range(4):
            tile = rows[128 * s + 32 * a : 128 * s + 32 * a + 32]
            tile = (tile if a == 0 else pltpu.roll(tile, a * PICK, 1)).astype(BF16).reshape(4, 8, 128)
            isend[s, a] = tile
            if a == 0:
                passed[s, :, 0] = tile
    gathered[0] = tokens[...]

    pl.semaphore_wait(barrier, 10)

    for s in range(3):
        for a in (2, 1, 3):
            remote(
                isend.at[s, a], passed.at[s, :, a], i_send, i_recv, (peer(*offset_of(s, -a, 0, 0)), tp)
            ).start()

    def gather(c, lines):
        for s, (lo, width) in enumerate(SLICES):
            cols = pl.ds(lo, width)
            remote(
                tokens.at[lines, cols], gathered.at[c, lines, cols], g_send, g_recv,
                (peer(*offset_of(s, 0, 0, c)), tp),
            ).start()

    gather(1, pl.ds(0, TOK))
    gather(3, pl.ds(0, TOK))
    remote(passed.at[:, :, 0:3], passed.at[:, :, 1:4], i_send, i_recv, partner).wait_recv()
    for s in range(3):
        for b in (2, 1, 3):
            remote(
                passed.at[s, b], irecv.at[s, b], j_send, j_recv, (peer(*offset_of(s, 0, -b, 0)), tp)
            ).start()
        irecv[s, 0] = passed[s, 0]
    gather(2, pl.ds(0, TOK))

    row = lax.broadcasted_iota(jnp.int32, (64, 128), 0)
    oy = (row >> 1) & 3
    ox = 2 * (((oy >> 1) + (row >> 3)) & 1) + (row & 1)
    oz = ((row >> 4) - oy - ox) & 3
    src = ((z - oz) & 3) * 16 + ((y - oy) & 3) * 4 + ((x - ox) & 3)
    src = jnp.concatenate([src] * (CAP // 128), axis=1)
    left = jnp.where(jnp.broadcast_to(home, (64, CAP)) == src, jnp.broadcast_to(score[...], (64, CAP)), 0.0)
    ordered = jnp.zeros((64, 128), F32)
    for _ in range(3):
        term = left.astype(BF16)
        ordered += jnp.dot(term, spread, preferred_element_type=F32)
        left -= term.astype(F32)
    upright = ordered.T
    for o in range(64):
        scale[o * PICK : (o + 1) * PICK, :] = jnp.broadcast_to(upright[0:PICK, o : o + 1], (PICK, 128))

    remote(irecv.at[:, 0:3], irecv.at[:, 1:4], j_send, j_recv, partner).wait_recv()
    token_row = lax.broadcasted_iota(jnp.int32, (TOK, 128), 0).astype(F32)

    def dispatch(r, c):
        for s, (lo, width) in enumerate(SLICES):
            cols = pl.ds(lo, width)
            total = irecv[s, (r - c) % 4, 0].astype(F32)
            for a in range(1, 4):
                total += irecv[s, (r - c - a) % 4, a].astype(F32)
            wanted = jnp.broadcast_to(total[c : c + 1] - 1.0, (TOK, 128))
            chosen_rows = jnp.where(wanted == token_row, 1.0, 0.0).astype(BF16)
            pick[(s * 4 + r) * 4 + c] = chosen_rows
            rows = lax.dot_general(
                chosen_rows, gathered[c, :, lo : lo + width],
                (((0,), (0,)), ((), ())), preferred_element_type=F32,
            ).astype(BF16)
            for a in range(4):
                b = (r - c - a) % 4
                blk = r * 16 + block_of(s, a, b, c)
                if a == 0 and b == 0:
                    own[blk, :, lo : lo + width] = rows[0:PICK]
                else:
                    dsend[blk, :, lo : lo + width] = rows[a * PICK : (a + 1) * PICK]

    def send_out(r, directions):
        for half in range(2):
            for c in directions:
                for a in range(4):
                    for s, (lo, width) in enumerate(SLICES):
                        b = (r - c - a) % 4
                        if (a == 0 and b == 0) or half_of(s, a, b, c) != half:
                            continue
                        blk, cols = r * 16 + block_of(s, a, b, c), pl.ds(lo, width)
                        remote(
                            dsend.at[blk, :, cols], own.at[blk, :, cols], d_send, d_recv.at[2 * r + half, s],
                            (peer(*offset_of(s, a, b, 0)), tp),
                        ).start()

    for r in range(2):
        dispatch(r, 0)
        send_out(r, (0,))
    remote(gathered.at[0:3], gathered.at[1:4], g_send, g_recv, partner).wait_recv()
    for r in range(4):
        rest = (1, 3, 2) if r < 2 else (0, 1, 3, 2)
        for c in rest:
            dispatch(r, c)
        send_out(r, rest)

    def forward(k):
        part = pl.ds(k * 8, 8)
        return remote(own.at[part], other.at[part], f_send, f_recv.at[k], partner)

    def pass_partial(k):
        return remote(psend.at[k], precv.at[k], p_send, p_recv.at[k], partner)

    def arrived(k):
        r, half = k // 2, k % 2
        for s, (lo, width) in enumerate(SLICES):
            count = 8 - (half_of(s, 0, 0, r) == half)
            part = own.at[pl.ds(k * 8, count), :, pl.ds(lo, width)]
            remote(part, part, d_send, d_recv.at[k, s], partner).wait_recv()

    def finish(k):
        r, half = k // 2, k % 2
        pass_partial(k).wait_recv()
        factor = jnp.concatenate([scale[k * PART : (k + 1) * PART, :]] * 4, axis=1)
        for n in range(2):
            cols = slice(n * 512, n * 512 + 512)
            summed = pown[k, :, cols].astype(F32) + precv[k, :, cols].astype(F32)
            wt[k * 8 : k * 8 + 8, :, cols] = (summed * factor).astype(BF16).reshape(8, PICK, 512)
        for n in range(3):
            if n == 0 or k != 6:
                send_back(k, n)
            if n == 0 and k == 7:
                send_back(6, 1)
                send_back(6, 2)

    def send_back(k, s):
        r, half = k // 2, k % 2
        lo, width = SLICES[s]
        cols = pl.ds(lo, width)
        for a in range(4):
            for b in range(4):
                c = (r - a - b) % 4
                if half_of(s, a, b, c) != half:
                    continue
                blk, place = r * 16 + block_of(s, a, b, c), r * 16 + c * 4 + a
                if a == 0 and b == 0:
                    ret[place, :, lo : lo + width] = wt[blk, :, lo : lo + width]
                    continue
                remote(
                    wt.at[blk, :, cols], ret.at[place, :, cols], r_send, r_recv.at[r, s],
                    (peer(*offset_of(s, -a, -b, 0)), tp),
                ).start()

    for copy in weights:
        copy.wait()
    mine_at = pl.multiple_of(tp * HALF, HALF)
    other_at = pl.multiple_of((1 - tp) * HALF, HALF)

    tiles_of = [slice(n * 256, (n + 1) * 256) for n in range(4)]

    def up_own(k):
        rows = own[k * 8 : k * 8 + 8].reshape(PART, HALF)
        for cols in tiles_of:
            gate_acc[:, cols] = jnp.dot(rows, wg[pl.ds(mine_at, HALF), cols], preferred_element_type=F32)
            up_acc[:, cols] = jnp.dot(rows, wu[pl.ds(mine_at, HALF), cols], preferred_element_type=F32)

    def up_other(k):
        rows = other[k * 8 : k * 8 + 8].reshape(PART, HALF)
        for cols in tiles_of:
            gate = gate_acc[:, cols] + jnp.dot(rows, wg[pl.ds(other_at, HALF), cols], preferred_element_type=F32)
            up = up_acc[:, cols] + jnp.dot(rows, wu[pl.ds(other_at, HALF), cols], preferred_element_type=F32)
            hidden[:, cols] = (gate / (1.0 + jnp.exp(-gate)) * up).astype(BF16)

    def down(k):
        for n, cols in enumerate(tiles_of):
            at = pl.multiple_of(other_at + n * 256, 256)
            psend[k, :, cols] = jnp.dot(
                hidden[...], wd[:, pl.ds(at, 256)], preferred_element_type=F32
            ).astype(BF16)
        pass_partial(k).start()
        for n, cols in enumerate(tiles_of):
            at = pl.multiple_of(mine_at + n * 256, 256)
            pown[k, :, cols] = jnp.dot(
                hidden[...], wd[:, pl.ds(at, 256)], preferred_element_type=F32
            ).astype(BF16)

    for k in range(8):
        arrived(k)
        forward(k).start()
        up_own(k)
        if k:
            down(k - 1)
        forward(k).wait_recv()
        up_other(k)
        if k:
            finish(k - 1)
    down(7)
    finish(7)

    sums[...] = jnp.zeros_like(sums)

    def combine(r, s):
        lo, width = SLICES[s]
        part = ret.at[pl.ds(r * 16, 15), :, pl.ds(lo, width)]
        remote(part, part, r_send, r_recv.at[r, s], partner).wait_recv()
        for c in range(4):
            rows = ret[pl.ds(r * 16 + c * 4, 4), :, lo : lo + width].reshape(4 * PICK, width)
            rows = jnp.concatenate([rows, jnp.zeros((128 - 4 * PICK, width), BF16)], axis=0)
            sums[c, :, lo : lo + width] += jnp.dot(
                pick[(s * 4 + r) * 4 + c], rows, preferred_element_type=F32
            )

    def combine_all(r, carry):
        for s in range(3):
            combine(r, s)
        return carry

    lax.fori_loop(0, 3, combine_all, 0)
    for s, (lo, width) in enumerate(SLICES):
        combine(3, s)
        cols = pl.ds(lo, width)
        for c in (2, 1, 3):
            rsend[c - 1, :, lo : lo + width] = sums[c, :, lo : lo + width].astype(BF16)
            remote(
                rsend.at[c - 1, :, cols], rrecv.at[c - 1, :, cols], q_send, q_recv.at[s],
                (peer(*offset_of(s, 0, 0, -c)), tp),
            ).start()
    for s, (lo, width) in enumerate(SLICES):
        part = rrecv.at[:, :, pl.ds(lo, width)]
        remote(part, part, q_send, q_recv.at[s], partner).wait_recv()
        total = sums[0, :, lo : lo + width]
        for c in range(3):
            total += rrecv[c, :, lo : lo + width].astype(F32)
        out[:, lo : lo + width] = total.astype(BF16)

    remote(passed.at[:, :, 0:3], passed.at[:, :, 1:4], i_send, i_recv, partner).wait_send()
    remote(irecv.at[:, 0:3], irecv.at[:, 1:4], j_send, j_recv, partner).wait_send()
    remote(gathered.at[0:3], gathered.at[1:4], g_send, g_recv, partner).wait_send()
    remote(dsend.at[0:60], dsend.at[0:60], d_send, d_recv.at[0, 0], partner).wait_send()
    remote(own, other, f_send, f_recv.at[0], partner).wait_send()
    remote(psend, precv, p_send, p_recv.at[0], partner).wait_send()
    remote(wt.at[0:60], ret.at[0:60], r_send, r_recv.at[0, 0], partner).wait_send()
    remote(rsend, rrecv, q_send, q_recv.at[0], partner).wait_send()


def on_device(tokens, chosen, gate_score, gate_weight, up_weight, down_weight):
    vmem = pl.BlockSpec(memory_space=pltpu.VMEM)
    hbm = pl.BlockSpec(memory_space=pl.ANY)
    dma = pltpu.SemaphoreType.DMA
    blocks = pltpu.VMEM((64, PICK, HALF), BF16)
    partial = pltpu.VMEM((8, PART, HALF), BF16)
    tiles = pltpu.VMEM((3, 4, 4, 8, 128), BF16)
    return pl.pallas_call(
        kernel,
        out_shape=jax.ShapeDtypeStruct((TOK, HALF), BF16),
        in_specs=[vmem, vmem, vmem, hbm, hbm, hbm],
        out_specs=vmem,
        scratch_shapes=[
            pltpu.VMEM((2048, 1024), BF16), pltpu.VMEM((2048, 1024), BF16), pltpu.VMEM((1024, 2048), BF16),
            pltpu.VMEM((4, TOK, HALF), BF16),
            tiles, tiles, tiles,
            pltpu.VMEM((48, TOK, 128), BF16),
            blocks, blocks, blocks,
            pltpu.VMEM((PART, 1024), F32), pltpu.VMEM((PART, 1024), F32), pltpu.VMEM((PART, 1024), BF16),
            partial, partial, partial,
            blocks, blocks,
            pltpu.VMEM((4, TOK, HALF), F32),
            pltpu.VMEM((3, TOK, HALF), BF16), pltpu.VMEM((3, TOK, HALF), BF16),
            pltpu.VMEM((64 * PICK, 128), F32),
            dma((3,)), dma, dma, dma, dma, dma, dma, dma, dma((8, 3)), dma, dma((8,)), dma, dma((8,)),
            dma, dma((4, 3)), dma, dma((3,)),
        ],
        compiler_params=pltpu.CompilerParams(
            collective_id=0, has_side_effects=True, vmem_limit_bytes=63 << 20
        ),
        cost_estimate=pl.CostEstimate(flops=20_000_000_000, bytes_accessed=14_000_000, transcendentals=1_600_000),
    )(tokens, chosen, gate_score, gate_weight[0], up_weight[0], down_weight[0])


def solution(mesh):
    in_specs = (
        P("ep", "tp"),
        P("ep", None),
        P("ep", None),
        P("ep", None, "tp"),
        P("ep", None, "tp"),
        P("ep", "tp", None),
    )
    out_specs = P("ep", "tp")
    return jax.shard_map(
        on_device, mesh=mesh, in_specs=in_specs, out_specs=out_specs, check_vma=False
    )
```
